256 devices in a mesh: fs: 32 (over z, x), tp: 4 (over y), rep: 2 (over core).
Axes of the slice: x: 4, y: 4, z: 8, core: 2. Of those that a mesh axis runs over, the one named last changes fastest.
Arguments:
- grads: float32 [2, 2, 8192, 2048], P('rep', None, 'fs', 'tp'), may hold values from -50 to 50
- momentum: float32 [2, 8192, 2048], P('rep', 'fs', 'tp'), may hold values from -14 to 14
Outputs:
- new_momentum: float32 [2, 8192, 2048], P('rep', 'fs', 'tp')
- step_matrix: float32 [2, 8192, 2048], P('rep', 'fs', 'tp')
The draws below stay inside these ranges and needn't reach their ends.
All inputs are finite; a program needn't handle non-finite values.
Results may differ from the reference program's by a relative error of at most 0.0003.
Values sent between devices are 32-bit elements; how exact they have to be, the bound alone decides.
No kernel may reach another device: no remote copies, remote signals or barrier semaphores. Data moves between devices by JAX's collectives and lax.ppermute only.
A program may use at most 64 MiB of HBM per device.

```python
import math
import jax
import jax.numpy as jnp
from jax import lax

D = 2048
FF = 8192
MATS = 2
ITERS = 3
REPLICAS = 2


def region_profile(key):
    inner = jax.random.fold_in(key, 71)
    phases = jax.random.uniform(inner, (MATS, 2), jnp.float32, 0.0, 2.0 * math.pi)
    rows = jnp.arange(FF, dtype=jnp.float32) / FF
    cols = jnp.arange(D, dtype=jnp.float32) / D
    row_part = jnp.exp(0.6 * jnp.sin(2.0 * math.pi * 1.5 * rows[None, :] + phases[:, 0:1]))
    col_part = jnp.exp(0.6 * jnp.sin(2.0 * math.pi * 1.25 * cols[None, :] + phases[:, 1:2]))
    return row_part[:, :, None] * col_part[:, None, :]


def draw_grads(key, part):
    profile = region_profile(key)
    own_part = jax.random.truncated_normal(key, -4.0, 4.0, (REPLICAS, MATS, FF, D), jnp.float32)
    return own_part * profile[None]


def draw_momentum(key, part):
    profile = region_profile(key)
    inner = jax.random.fold_in(key, 29)
    return jax.random.truncated_normal(inner, -4.0, 4.0, (MATS, FF, D), jnp.float32) * profile


def setup_inputs(seed: int = 0) -> dict:
    arg_keys = jax.random.split(jax.random.key(seed), 3)
    return {
        "grads": draw_grads(jax.random.fold_in(arg_keys[2], 71), 0),
        "momentum": draw_momentum(jax.random.fold_in(arg_keys[2], 71), 0),
    }


momentum_decay = 0.95
norm_spread = 2.56
poly_linear = 3.4445
poly_cubic = -4.775
poly_quintic = 2.0315
highest = lax.Precision.HIGHEST

def orthogonalize(moment):
    squares = jnp.sum(moment * moment)
    scaling = jnp.sqrt(norm_spread * squares / D + 1.0)
    current = moment / scaling
    update = current
    for sweep in range(ITERS):
        gram = jnp.dot(current.T, current, precision=highest, preferred_element_type=jnp.float32)
        squared = jnp.dot(gram, gram, precision=highest, preferred_element_type=jnp.float32)
        factor = poly_cubic * gram + poly_quintic * squared
        update = poly_linear * current + jnp.dot(current, factor, precision=highest, preferred_element_type=jnp.float32)
        current = update
    return update * math.sqrt(FF)

def reference(grads, momentum):
    total = lax.optimization_barrier(jnp.sum(grads, axis=0))
    new_momentum = momentum_decay * momentum + total
    steps = jnp.stack([orthogonalize(new_momentum[index]) for index in range(MATS)])
    return (new_momentum, steps)
```

```python
import functools
import math

import jax
import jax.numpy as jnp
from jax import lax
from jax.experimental import pallas as pl
from jax.experimental.pallas import tpu as pltpu
from jax.sharding import Mesh
from jax.sharding import PartitionSpec as P

D = 2048
FF = 8192
Z, X, Y = 8, 4, 4
ROWS = D // Z
COLS = D // (X * Y)
EXTRA = 8

momentum_decay = 0.95
norm_spread = 2.56
linear = 3.4445
cubic = -4.775
quintic = 2.0315


f32, bf16 = jnp.float32, jnp.bfloat16
VMEM = pl.BlockSpec(memory_space=pltpu.VMEM)
SMEM = pl.BlockSpec(memory_space=pltpu.SMEM)


def halves(a):
    high = a.astype(bf16)
    return high, (a - high.astype(f32)).astype(bf16)


def dot(a, b, dims=((1,), (0,))):
    return lax.dot_general(a, b, (dims, ((), ())), preferred_element_type=f32)


def product(a, b, dims=((1,), (0,))):
    (ah, al), (bh, bl) = halves(a), halves(b)
    n = b.shape[1]
    if n == COLS:
        both = dot(ah, jnp.concatenate([bh, bl], 1), dims)
        return both[:, :n] + (both[:, n:] + dot(al, bh, dims))
    return dot(ah, bh, dims) + (dot(ah, bl, dims) + dot(al, bh, dims))


def eye(first_row, first_col):
    rows = lax.broadcasted_iota(jnp.int32, (ROWS, COLS), 0) + first_row
    cols = lax.broadcasted_iota(jnp.int32, (ROWS, COLS), 1) + first_col
    return jnp.where(rows == cols, jnp.float32(linear), jnp.float32(0))


def call(kernel, outs, *args, flops=400_000_000):
    specs = [SMEM if a.dtype == jnp.int32 else VMEM for a in args]
    return pl.pallas_call(
        kernel,
        out_shape=[jax.ShapeDtypeStruct(s, f32) for s in outs],
        in_specs=specs,
        out_specs=[VMEM] * len(outs),
        cost_estimate=pl.CostEstimate(flops=flops, bytes_accessed=4_000_000, transcendentals=0),
    )(*args)


def tile_product(row, col):
    def step(i, total):
        a = jnp.concatenate([row(2 * i), row(2 * i + 1)], 1)
        return total + product(a, col(i))

    return lax.fori_loop(0, Z, step, jnp.zeros((ROWS, COLS), f32))


def fill(ref, value):
    for n in range(ref.shape[0]):
        ref[n] = value


def gram_kernel(full, own, out):
    mine = own[...]
    squares = jnp.sum(mine * mine)
    for y in range(Y):
        part = product(full[y], mine, ((0,), (0,)))
        for x in range(X):
            out[x, y * 512 : (y + 1) * 512, :] = part[:, x * COLS : (x + 1) * COLS]
    for x in range(X):
        out[x, D:, :] = jnp.full((EXTRA, COLS), squares, f32)


def sum_x_kernel(parts, out):
    for z in range(Z):
        rows = slice(z * ROWS, (z + 1) * ROWS)
        out[z, :ROWS, :] = (parts[0, rows] + parts[1, rows]) + (parts[2, rows] + parts[3, rows])
    extra = (parts[0, D:] + parts[1, D:]) + (parts[2, D:] + parts[3, D:])
    for z in range(Z):
        out[z, ROWS:, :] = extra


def sum_z_kernel(parts, out, tile):
    total = parts[0]
    for z in range(1, Z):
        total = total + parts[z]
    fill(out, total)
    tile[...] = total[:ROWS]


def square_first_kernel(row, col, out, scale):
    squares = jnp.zeros((EXTRA, COLS), f32)
    for n in range(X * Y):
        squares = squares + row[n, ROWS:, :]
    squares = squares * (1.0 / X)
    scaling = jnp.sqrt(norm_spread * squares / D + 1.0)
    scale[...] = 1.0 / scaling
    inverse = jnp.max(1.0 / (scaling * scaling))
    total = tile_product(lambda j: row[j, :ROWS, :], lambda i: col[i]) * (inverse * inverse)
    fill(out, total)


def inverse_square(scale):
    s = jnp.max(scale[...])
    return s * s


def times_poly_first_kernel(row, tile, scol, scale, where, out):
    inverse = inverse_square(scale)
    total = tile_product(lambda j: row[j, :ROWS, :], lambda i: scol[i]) * inverse
    h = linear * (tile[...] * inverse) + (cubic * scol[where[0]] + quintic * total)
    fill(out, h)


def next_gram_kernel(hrow, col, scol, scale, where, out, tile, pcol):
    inverse = inverse_square(scale)
    first_col = where[1] * COLS
    for i in range(Z):
        pcol[i] = eye(i * ROWS, first_col) + (cubic * (col[i] * inverse) + quintic * scol[i])
    total = tile_product(lambda j: hrow[j], lambda i: pcol[i])
    fill(out, total)
    tile[...] = total


def square_kernel(row, col, out):
    fill(out, tile_product(lambda j: row[j], lambda i: col[i]))


def poly_products_kernel(row, col, srow, pcol, where, hout, pout, prow):
    first_row = where[0] * ROWS
    for j in range(X * Y):
        prow[j] = eye(first_row, j * COLS) + (cubic * row[j] + quintic * srow[j])
    fill(hout, tile_product(lambda j: prow[j], lambda i: col[i]))
    fill(pout, tile_product(lambda j: prow[j], lambda i: pcol[i]))


def gram_second_kernel(prow, hcol, out, tile):
    total = tile_product(lambda j: prow[j], lambda i: hcol[i])
    fill(out, total)
    tile[...] = total


def last_poly_kernel(prow, col, scol, scale, where, out):
    first_col = where[1] * COLS

    def pcol(i):
        return eye(i * ROWS, first_col) + (cubic * col[i] + quintic * scol[i])

    total = tile_product(lambda j: prow[j], pcol) * (jnp.max(scale[...]) * math.sqrt(FF))
    fill(out, total)


def apply_kernel(full, q, out):
    for x in range(X):
        total = jnp.zeros((ROWS, COLS), f32)
        for y in range(Y):
            total = total + product(full[y], q[x, y * 512 : (y + 1) * 512, :])
        out[:, x * COLS : (x + 1) * COLS] = total


def exchange(parts, axes):
    return lax.all_to_all(parts, axes, 0, 0, tiled=True)


def z_direct(tile):
    me = lax.axis_index("z")
    blocks = [tile] + [
        lax.ppermute(tile, "z", [(i, (i + d) % Z) for i in range(Z)]) for d in range(1, Z)
    ]
    panel = jnp.zeros((Z, ROWS, COLS), f32)
    for d in range(Z):
        panel = lax.dynamic_update_slice(panel, blocks[d][None], (lax.rem(me - d + Z, Z), 0, 0))
    return panel


def per_device(grads, momentum):
    me = lax.axis_index("rep")
    theirs = lax.dynamic_index_in_dim(grads[0], 1 - me, 0, keepdims=False)
    mine = lax.dynamic_index_in_dim(grads[0], me, 0, keepdims=False)
    moment = momentum_decay * momentum[0] + (mine + lax.ppermute(theirs, "rep", [(0, 1), (1, 0)]))

    tile_shape, bcast_xy, bcast_z = (ROWS, COLS), (X * Y, ROWS, COLS), (Z, ROWS, COLS)
    where = jnp.stack([lax.axis_index("z"), lax.axis_index("y") * X + lax.axis_index("x")]).astype(jnp.int32)

    full = exchange(jnp.broadcast_to(moment[None], (Y, *moment.shape)), "y")
    (parts,) = call(gram_kernel, [(X, D + EXTRA, COLS)], full, moment, flops=2_000_000_000)
    parts = exchange(parts, "x")
    (parts,) = call(sum_x_kernel, [(Z, ROWS + EXTRA, COLS)], parts)
    parts = exchange(parts, "z")
    out, tile = call(sum_z_kernel, [(X * Y, ROWS + EXTRA, COLS), tile_shape], parts)

    row, col = exchange(out, ("y", "x")), z_direct(tile)
    out, scale = call(square_first_kernel, [bcast_z, (EXTRA, COLS)], row, col)
    scol = exchange(out, "z")
    (out,) = call(times_poly_first_kernel, [bcast_xy], row, tile, scol, scale, where)
    hrow = exchange(out, ("y", "x"))
    out, tile, pcol = call(next_gram_kernel, [bcast_xy, tile_shape, bcast_z], hrow, col, scol, scale, where)

    row, col = exchange(out, ("y", "x")), z_direct(tile)
    (out,) = call(square_kernel, [bcast_xy], row, col)
    srow = exchange(out, ("y", "x"))
    hout, pout, prow = call(poly_products_kernel, [bcast_z, bcast_xy, bcast_xy], row, col, srow, pcol, where)
    hcol = exchange(hout, "z")
    out, tile = call(gram_second_kernel, [bcast_xy, tile_shape], prow, hcol)
    both_row = exchange(pout, ("y", "x"))

    row, col = exchange(out, ("y", "x")), z_direct(tile)
    (out,) = call(square_kernel, [bcast_z], row, col)
    scol = exchange(out, "z")
    (out,) = call(last_poly_kernel, [bcast_z], both_row, col, scol, scale, where)

    q = exchange(out, "z").reshape(D, COLS)
    q = exchange(jnp.broadcast_to(q[None], (X, D, COLS)), "x")
    (step,) = call(apply_kernel, [(256, 512)], full, q, flops=2_000_000_000)
    return moment[None], step[None]


def solution(mesh):
    torus = Mesh(
        mesh.devices.reshape(Z, X, Y, mesh.shape["rep"]),
        ("z", "x", "y", "rep"),
    )
    in_specs = (P("rep", None, ("z", "x"), "y"), P("rep", ("z", "x"), "y"))
    out_specs = (P("rep", ("z", "x"), "y"), P("rep", ("z", "x"), "y"))
    return jax.shard_map(
        per_device, mesh=torus, in_specs=in_specs, out_specs=out_specs, check_vma=False
    )
```

```python
import functools
import math

import jax
import jax.numpy as jnp
from jax import lax
from jax.experimental import pallas as pl
from jax.experimental.pallas import tpu as pltpu
from jax.sharding import Mesh
from jax.sharding import PartitionSpec as P

D = 2048
FF = 8192
Z, X, Y = 8, 4, 4
ROWS = D // Z
COLS = D // (X * Y)
EXTRA = 8

momentum_decay = 0.95
norm_spread = 2.56
linear = 3.4445
cubic = -4.775
quintic = 2.0315


f32, bf16 = jnp.float32, jnp.bfloat16
VMEM = pl.BlockSpec(memory_space=pltpu.VMEM)
SMEM = pl.BlockSpec(memory_space=pltpu.SMEM)


def split(a):
    high = a.astype(bf16)
    rest = a - high.astype(f32)
    middle = rest.astype(bf16)
    return high, middle, (rest - middle.astype(f32)).astype(bf16)


def dot(a, b, dims=((1,), (0,))):
    return lax.dot_general(a, b, (dims, ((), ())), preferred_element_type=f32)


def product(a, b, dims=((1,), (0,))):
    a1, a2, a3 = split(a)
    b1, b2, b3 = split(b)
    n = b.shape[1]
    if n == COLS:
        pair = jnp.concatenate([b1, b2], 1)
        upper, lower = dot(a1, pair, dims), dot(a2, pair, dims)
        small = dot(a1, b3, dims) + (dot(a3, b1, dims) + lower[:, n:])
        return upper[:, :n] + (small + (upper[:, n:] + lower[:, :n]))
    small = dot(a1, b3, dims) + (dot(a3, b1, dims) + dot(a2, b2, dims))
    return dot(a1, b1, dims) + (small + (dot(a1, b2, dims) + dot(a2, b1, dims)))


def eye(first_row, first_col):
    rows = lax.broadcasted_iota(jnp.int32, (ROWS, COLS), 0) + first_row
    cols = lax.broadcasted_iota(jnp.int32, (ROWS, COLS), 1) + first_col
    return jnp.where(rows == cols, jnp.float32(linear), jnp.float32(0))


def call(kernel, outs, *args, flops=800_000_000, cols=0):
    specs = [SMEM if a.dtype == jnp.int32 else VMEM for a in args]
    return pl.pallas_call(
        kernel,
        out_shape=[jax.ShapeDtypeStruct(s, f32) for s in outs],
        in_specs=specs,
        out_specs=[VMEM] * len(outs),
        scratch_shapes=[pltpu.VMEM((Z, ROWS, cols * COLS), f32)] if cols else [],
        cost_estimate=pl.CostEstimate(flops=flops, bytes_accessed=4_000_000, transcendentals=0),
    )(*args)


def block(where, n):
    step = (n + 1) // 2
    return lax.rem(where[0] + Z + jnp.where(n % 2 == 1, -step, step), Z)


def tile_products(where, panel, rows, cols):
    for n in range(Z):
        for c, col in enumerate(cols):
            panel[n, :, c * COLS : (c + 1) * COLS] = col[n][...]

    def step(n, totals):
        i = block(where, n)
        b = panel[n]
        return tuple(
            t + product(jnp.concatenate([row(2 * i), row(2 * i + 1)], 1), b) for t, row in zip(totals, rows)
        )

    zero = jnp.zeros((ROWS, len(cols) * COLS), f32)
    totals = lax.fori_loop(0, Z, step, (zero,) * len(rows))
    return [t[:, c * COLS : (c + 1) * COLS] for t in totals for c in range(len(cols))]


def fill(ref, value):
    for n in range(ref.shape[0]):
        ref[n] = value


def gram_kernel(full, own, out):
    mine = own[...]
    squares = jnp.sum(mine * mine)

    def step(y, carry):
        part = product(full[y], mine, ((0,), (0,)))
        for x in range(X):
            out[x, pl.ds(pl.multiple_of(y * 512, 512), 512), :] = part[:, x * COLS : (x + 1) * COLS]
        return carry

    lax.fori_loop(0, Y, step, 0)
    for x in range(X):
        out[x, D:, :] = jnp.full((EXTRA, COLS), squares, f32)


def sum_x_kernel(parts, out):
    for z in range(Z):
        rows = slice(z * ROWS, (z + 1) * ROWS)
        out[z, :ROWS, :] = (parts[0, rows] + parts[1, rows]) + (parts[2, rows] + parts[3, rows])
    extra = (parts[0, D:] + parts[1, D:]) + (parts[2, D:] + parts[3, D:])
    for z in range(Z):
        out[z, ROWS:, :] = extra


def sum_z_kernel(parts, out, tile):
    total = parts[0]
    for z in range(1, Z):
        total = total + parts[z]
    fill(out, total)
    tile[...] = total[:ROWS]


def square_kernel(where, row, *refs):
    col, (out, tile, scale, panel) = refs[:Z], refs[Z:]
    squares = jnp.zeros((EXTRA, COLS), f32)
    for n in range(X * Y):
        squares = squares + row[n, ROWS:, :]
    squares = squares * (1.0 / X)
    scaling = jnp.sqrt(norm_spread * squares / D + 1.0)
    scale[...] = 1.0 / scaling
    inverse = jnp.max(1.0 / (scaling * scaling))
    (total,) = tile_products(where, panel, [lambda j: row[j, :ROWS, :]], [col])
    total = total * (inverse * inverse)
    fill(out, total)
    tile[...] = total


def poly_kernel(where, row, srow, scale, *refs):
    col, scol, (out, tile, prow, ptile, panel) = refs[:Z], refs[Z : 2 * Z], refs[2 * Z :]
    s = jnp.max(scale[...])
    inverse = s * s
    for j in range(X * Y):
        scaled = row[j, :ROWS, :] * inverse
        prow[j] = eye(where[0] * ROWS, j * COLS) + (cubic * scaled + quintic * srow[j])
    pcol = []
    for n in range(Z):
        scaled = col[n][...] * inverse
        first = eye(block(where, n) * ROWS, where[1] * COLS)
        pcol.append(first + (cubic * scaled + quintic * scol[n][...]))
    ptile[...] = pcol[0]
    h, w = tile_products(
        where, panel, [lambda j: row[j, :ROWS, :], lambda j: prow[j]], [pcol]
    )
    fill(out, w)
    tile[...] = h * inverse


def shared_column_kernel(where, left, right, *refs):
    col, (out, tile, other, panel) = refs[:Z], refs[Z:]
    first, second = tile_products(
        where, panel, [lambda j: left[j], lambda j: right[j]], [col]
    )
    fill(out, second)
    tile[...] = first
    other[...] = second


def second_poly_kernel(where, row, gtile, ptile, utile, *refs):
    hcol, col, (out, tile, panel) = refs[:Z], refs[Z : 2 * Z], refs[2 * Z :]
    squared, times = tile_products(where, panel, [lambda j: row[j]], [hcol, col])
    first = eye(where[0] * ROWS, where[1] * COLS)
    fill(out, first + (cubic * gtile[...] + quintic * squared))
    tile[...] = linear * ptile[...] + (cubic * utile[...] + quintic * times)


def shared_row_kernel(where, row, *refs):
    col, other, (out, tile, panel) = refs[:Z], refs[Z : 2 * Z], refs[2 * Z :]
    first, second = tile_products(where, panel, [lambda j: row[j]], [col, other])
    fill(out, second)
    tile[...] = first


def last_kernel(where, row, both, vtile, scale, *refs):
    col, (out, panel) = refs[:Z], refs[Z:]
    (total,) = tile_products(where, panel, [lambda j: row[j]], [col])
    total = linear * both[...] + (cubic * vtile[...] + quintic * total)
    fill(out, total * (jnp.max(scale[...]) * math.sqrt(FF)))


def apply_kernel(full, q, out):
    def step(y, total):
        rows = pl.ds(pl.multiple_of(y * 512, 512), 512)
        (a1, a2, _), (b1, b2, _) = split(full[y]), split(jnp.concatenate([q[x, rows, :] for x in range(X)], 1))
        return total + (dot(a1, b1) + (dot(a1, b2) + dot(a2, b1)))

    out[...] = lax.fori_loop(0, Y, step, jnp.zeros((256, 512), f32))


def exchange(parts, axes):
    return lax.all_to_all(parts, axes, 0, 0, tiled=True)


def z_ring(tile):
    up = [(i, (i + 1) % Z) for i in range(Z)]
    down = [(i, (i - 1) % Z) for i in range(Z)]
    blocks, low, high = [tile], tile, tile
    for _ in range(3):
        low, high = lax.ppermute(low, "z", up), lax.ppermute(high, "z", down)
        blocks += [low, high]
    return blocks + [lax.ppermute(high, "z", down)]


def per_device(grads, momentum):
    me = lax.axis_index("rep")
    theirs = lax.dynamic_index_in_dim(grads[0], 1 - me, 0, keepdims=False)
    mine = lax.dynamic_index_in_dim(grads[0], me, 0, keepdims=False)
    moment = momentum_decay * momentum[0] + (mine + lax.ppermute(theirs, "rep", [(0, 1), (1, 0)]))

    tile_shape, bcast_xy, bcast_z = (ROWS, COLS), (X * Y, ROWS, COLS), (Z, ROWS, COLS)
    where = jnp.stack([lax.axis_index("z"), lax.axis_index("y") * X + lax.axis_index("x")]).astype(jnp.int32)

    full = exchange(jnp.broadcast_to(moment[None], (Y, *moment.shape)), "y")
    (parts,) = call(gram_kernel, [(X, D + EXTRA, COLS)], full, moment, flops=2_000_000_000)
    parts = exchange(parts, "x")
    (parts,) = call(sum_x_kernel, [(Z, ROWS + EXTRA, COLS)], parts)
    parts = exchange(parts, "z")
    out, tile = call(sum_z_kernel, [(X * Y, ROWS + EXTRA, COLS), tile_shape], parts)

    def gather(out, tile):
        return exchange(out, ("y", "x")), z_ring(tile)

    row, col = gather(out, tile)
    out, tile, scale = call(square_kernel, [bcast_xy, tile_shape, (EXTRA, COLS)], where, row, *col, cols=1)
    srow, scol = gather(out, tile)
    out, tile, prow, ptile = call(
        poly_kernel,
        [bcast_xy, tile_shape, bcast_xy, tile_shape],
        where, row, srow, scale, *col, *scol, cols=1,
    )
    wrow, hcol = gather(out, tile)
    out, gtile, utile = call(
        shared_column_kernel, [bcast_xy, tile_shape, tile_shape], where, prow, wrow, *hcol, cols=1
    )
    urow, gcol = gather(out, gtile)
    out, both = call(
        second_poly_kernel, [bcast_xy, tile_shape], where, urow, gtile, ptile, utile, *hcol, *gcol, cols=2
    )
    prow, bothcol = gather(out, both)
    out, tile = call(
        shared_row_kernel, [bcast_xy, tile_shape], where, prow, *gcol, *bothcol, cols=2
    )
    xrow, hcol = gather(out, tile)
    out, gtile, vtile = call(
        shared_column_kernel, [bcast_xy, tile_shape, tile_shape], where, prow, xrow, *hcol, cols=1
    )
    vrow, gcol = gather(out, gtile)
    (out,) = call(last_kernel, [bcast_z], where, vrow, both, vtile, scale, *gcol, cols=1)

    q = exchange(out, "z").reshape(D, COLS)
    q = exchange(jnp.broadcast_to(q[None], (X, D, COLS)), "x")
    (step,) = call(apply_kernel, [(256, 512)], full, q, flops=2_000_000_000)
    return moment[None], step[None]


def solution(mesh):
    torus = Mesh(
        mesh.devices.reshape(Z, X, Y, mesh.shape["rep"]),
        ("z", "x", "y", "rep"),
    )
    in_specs = (P("rep", None, ("z", "x"), "y"), P("rep", ("z", "x"), "y"))
    out_specs = (P("rep", ("z", "x"), "y"), P("rep", ("z", "x"), "y"))
    return jax.shard_map(
        per_device, mesh=torus, in_specs=in_specs, out_specs=out_specs, check_vma=False
    )
```

```python
import functools
import math

import jax
import jax.numpy as jnp
from jax import lax
from jax.experimental import pallas as pl
from jax.experimental.pallas import tpu as pltpu
from jax.sharding import Mesh
from jax.sharding import PartitionSpec as P

D = 2048
FF = 8192
Z, X, Y = 8, 4, 4
ROWS = D // Z
COLS = D // (X * Y)
EXTRA = 8

momentum_decay = 0.95
norm_spread = 2.56
linear = 3.4445
cubic = -4.775
quintic = 2.0315


f32, bf16 = jnp.float32, jnp.bfloat16
VMEM = pl.BlockSpec(memory_space=pltpu.VMEM)
SMEM = pl.BlockSpec(memory_space=pltpu.SMEM)


def split(a):
    high = a.astype(bf16)
    rest = a - high.astype(f32)
    middle = rest.astype(bf16)
    return high, middle, (rest - middle.astype(f32)).astype(bf16)


def dot(a, b, dims=((1,), (0,))):
    return lax.dot_general(a, b, (dims, ((), ())), preferred_element_type=f32)


def product(a, b, dims=((1,), (0,))):
    a1, a2, a3 = split(a)
    b1, b2, b3 = split(b)
    n = b.shape[1]
    if n == COLS:
        pair = jnp.concatenate([b1, b2], 1)
        upper, lower = dot(a1, pair, dims), dot(a2, pair, dims)
        small = dot(a1, b3, dims) + (dot(a3, b1, dims) + lower[:, n:])
        return upper[:, :n] + (small + (upper[:, n:] + lower[:, :n]))
    small = dot(a1, b3, dims) + (dot(a3, b1, dims) + dot(a2, b2, dims))
    return dot(a1, b1, dims) + (small + (dot(a1, b2, dims) + dot(a2, b1, dims)))


def eye(first_row, first_col):
    rows = lax.broadcasted_iota(jnp.int32, (ROWS, COLS), 0) + first_row
    cols = lax.broadcasted_iota(jnp.int32, (ROWS, COLS), 1) + first_col
    return jnp.where(rows == cols, jnp.float32(linear), jnp.float32(0))


def call(kernel, outs, *args, flops=800_000_000, scratch=None, limit=20, dtype=f32):
    specs = [SMEM if a.dtype == jnp.int32 else VMEM for a in args]
    return pl.pallas_call(
        kernel,
        out_shape=[jax.ShapeDtypeStruct(s, dtype) for s in outs],
        in_specs=specs,
        out_specs=[VMEM] * len(outs),
        scratch_shapes=[pltpu.VMEM(scratch, f32)] if scratch else [],
        compiler_params=pltpu.CompilerParams(vmem_limit_bytes=limit << 20),
        cost_estimate=pl.CostEstimate(flops=flops, bytes_accessed=4_000_000, transcendentals=0),
    )(*args)


def block(where, n):
    step = (n + 1) // 2
    return lax.rem(where[0] + Z + jnp.where(n % 2 == 1, -step, step), Z)


def tile_products(where, panel, rows, cols):
    for n in range(Z):
        for c, col in enumerate(cols):
            panel[n, :, c * COLS : (c + 1) * COLS] = col[n][...]

    def step(n, totals):
        i = block(where, n)
        b = panel[n]
        return tuple(
            t + product(jnp.concatenate([row(2 * i), row(2 * i + 1)], 1), b) for t, row in zip(totals, rows)
        )

    zero = jnp.zeros((ROWS, len(cols) * COLS), f32)
    totals = lax.fori_loop(0, Z, step, (zero,) * len(rows))
    return [t[:, c * COLS : (c + 1) * COLS] for t in totals for c in range(len(cols))]


def loop(count, body):
    def step(n, carry):
        body(n)
        return carry

    lax.fori_loop(0, count, step, 0)


def fill(ref, value):
    def store(n):
        ref[n] = value

    loop(ref.shape[0], store)


def gram_part(other, mine, out, first):
    for half in range(2):
        part = product(other[:, half * 256 : (half + 1) * 256], mine, ((0,), (0,)))
        rows = slice(first + half * 256, first + (half + 1) * 256)
        for x in range(X):
            out[x, rows, :] = part[:, x * COLS : (x + 1) * COLS]


def gram_own_kernel(own, out):
    mine = own[...]
    gram_part(mine, mine, out, 0)
    squares = jnp.sum(mine * mine)
    for x in range(X):
        out[x, 512:, :] = jnp.full((EXTRA, COLS), squares, f32)


def gram_near_kernel(own, before, after, out, done, both):
    both[0] = before[...]
    both[1] = after[...]
    mine = own[...]

    def part(n):
        columns = pl.ds(pl.multiple_of(lax.rem(n, 2) * 256, 256), 256)
        part = product(both[n // 2, :, columns], mine, ((0,), (0,)))
        for x in range(X):
            out[x, pl.ds(pl.multiple_of(n * 256, 256), 256), :] = part[:, x * COLS : (x + 1) * COLS]

    loop(4, part)
    done[...] = jnp.zeros((EXTRA, COLS), f32)


def gram_far_kernel(own, upper, lower, done, out):
    gram_part(jnp.concatenate([upper[...], lower[...]], 0), own[...], out, 0)


def sum_x_kernel(where, own, near, far, out):
    def total(parts, first, count):
        rows = slice(first, first + count)
        return (parts[0, rows] + parts[1, rows]) + (parts[2, rows] + parts[3, rows])

    y = where[1] // X
    for parts, first, step in ((own, 0, 0), (near, 0, Y - 1), (near, 512, 1), (far, 0, 2)):
        for half in range(2):
            z = 2 * lax.rem(y + step, Y) + half
            out[z, :ROWS, :] = total(parts, first + half * ROWS, ROWS)
    extra = total(own, 512, EXTRA)
    for z in range(Z):
        out[z, ROWS:, :] = extra


def sum_z_kernel(parts, out, tile):
    total = parts[0]
    for z in range(1, Z):
        total = total + parts[z]
    fill(out, total)
    tile[...] = total[:ROWS]


def square_kernel(where, row, *refs):
    col, (out, tile, scale, panel) = refs[:Z], refs[Z:]
    squares = jnp.zeros((EXTRA, COLS), f32)
    for n in range(X * Y):
        squares = squares + row[n, ROWS:, :]
    squares = squares * (1.0 / X)
    scaling = jnp.sqrt(norm_spread * squares / D + 1.0)
    scale[...] = 1.0 / scaling
    inverse = jnp.max(1.0 / (scaling * scaling))
    (total,) = tile_products(where, panel, [lambda j: row[j, :ROWS, :]], [col])
    total = total * (inverse * inverse)
    fill(out, total)
    tile[...] = total


def poly_kernel(where, row, srow, scale, *refs):
    col, scol, (out, tile, prow, ptile, panel) = refs[:Z], refs[Z : 2 * Z], refs[2 * Z :]
    s = jnp.max(scale[...])
    inverse = s * s

    def poly_row(j):
        scaled = row[j, :ROWS, :] * inverse
        prow[j] = eye(where[0] * ROWS, j * COLS) + (cubic * scaled + quintic * srow[j])

    loop(X * Y, poly_row)
    pcol = []
    for n in range(Z):
        scaled = col[n][...] * inverse
        first = eye(block(where, n) * ROWS, where[1] * COLS)
        pcol.append(first + (cubic * scaled + quintic * scol[n][...]))
    ptile[...] = pcol[0]
    h, w = tile_products(
        where, panel, [lambda j: row[j, :ROWS, :], lambda j: prow[j]], [pcol]
    )
    fill(out, w)
    tile[...] = h * inverse


def shared_column_kernel(where, left, right, *refs):
    col, (out, tile, other, panel) = refs[:Z], refs[Z:]
    first, second = tile_products(
        where, panel, [lambda j: left[j], lambda j: right[j]], [col]
    )
    fill(out, second)
    tile[...] = first
    other[...] = second


def second_poly_kernel(where, row, gtile, ptile, utile, *refs):
    hcol, col, (out, tile, panel) = refs[:Z], refs[Z : 2 * Z], refs[2 * Z :]
    squared, times = tile_products(where, panel, [lambda j: row[j]], [hcol, col])
    first = eye(where[0] * ROWS, where[1] * COLS)
    fill(out, first + (cubic * gtile[...] + quintic * squared))
    tile[...] = linear * ptile[...] + (cubic * utile[...] + quintic * times)


def shared_row_kernel(where, row, *refs):
    col, other, (out, tile, panel) = refs[:Z], refs[Z : 2 * Z], refs[2 * Z :]
    first, second = tile_products(where, panel, [lambda j: row[j]], [col, other])
    fill(out, second)
    tile[...] = first


def last_kernel(where, row, both, vtile, scale, *refs):
    col, (out, panel) = refs[:Z], refs[Z:]
    (total,) = tile_products(where, panel, [lambda j: row[j]], [col])
    total = linear * both[...] + (cubic * vtile[...] + quintic * total)
    out[...] = total * (jnp.max(scale[...]) * math.sqrt(FF))


def prepare_kernel(where, own, before, after, upper, lower, high, low):
    y = where[1] // X
    for part, step in ((own[...], 0), (before[...], Y - 1), (after[...], 1), (None, 2)):
        if part is None:
            part = jnp.concatenate([upper[...], lower[...]], 0)
        first, second, _ = split(part)
        for half in range(2):
            i = 2 * lax.rem(y + step, Y) + half
            high[i] = first[:, half * 256 : (half + 1) * 256]
            low[i] = second[:, half * 256 : (half + 1) * 256]


def apply_kernel(where, high, low, *refs):
    upper, lower, (out, panel) = refs[:1], refs[1 : 1 + Z], refs[1 + Z :]
    for n in range(Z):
        for x in range(X):
            panel[n, :, x * COLS : (x + 1) * COLS] = lower[n][x]

    def step(n, total):
        i = block(where, n)
        first = jnp.concatenate([upper[0][x, n] for x in range(X)], 1)
        b1, b2, _ = split(jnp.concatenate([first, panel[n]], 0))
        return total + (dot(high[i], b1) + (dot(high[i], b2) + dot(low[i], b1)))

    out[...] = lax.fori_loop(0, Z, step, jnp.zeros((256, 512), f32))


def exchange(parts, axes):
    return lax.all_to_all(parts, axes, 0, 0, tiled=True)


def z_gather(tile):
    def from_offset(a, offset):
        return lax.ppermute(a, "z", [(i, (i - offset) % Z) for i in range(Z)])

    near = {o: from_offset(tile, o) for o in (1, -1, 2, -2)}
    far = from_offset(near[2], 2)
    return [tile, near[-1], near[1], near[-2], near[2], from_offset(near[-2], -1), from_offset(near[2], 1), far]


def per_device(grads, momentum):
    me = lax.axis_index("rep")
    theirs = lax.dynamic_index_in_dim(grads[0], 1 - me, 0, keepdims=False)
    mine = lax.dynamic_index_in_dim(grads[0], me, 0, keepdims=False)
    moment = momentum_decay * momentum[0] + (mine + lax.ppermute(theirs, "rep", [(0, 1), (1, 0)]))

    tile_shape, bcast_xy, bcast_z = (ROWS, COLS), (X * Y, ROWS, COLS), (Z, ROWS, COLS)
    where = jnp.stack([lax.axis_index("z"), lax.axis_index("y") * X + lax.axis_index("x")]).astype(jnp.int32)

    up, down = [(i, (i + 1) % Y) for i in range(Y)], [(i, (i - 1) % Y) for i in range(Y)]
    before, after = lax.ppermute(moment, "y", up), lax.ppermute(moment, "y", down)
    upper, lower = lax.ppermute(before[:128], "y", up), lax.ppermute(after[128:], "y", down)
    (own,) = call(gram_own_kernel, [(X, 512 + EXTRA, COLS)], moment)
    own = exchange(own, "x")
    near, done = call(
        gram_near_kernel,
        [(X, 1024, COLS), (EXTRA, COLS)],
        moment, before, after,
        flops=1_600_000_000, scratch=(2, 256, 512),
    )
    near = exchange(near, "x")
    (far,) = call(gram_far_kernel, [(X, 512, COLS)], moment, upper, lower, done)
    far = exchange(far, "x")
    rows = call(
        prepare_kernel, [(Z, ROWS, 256)] * 2, where, moment, before, after, upper, lower, dtype=bf16
    )
    (parts,) = call(sum_x_kernel, [(Z, ROWS + EXTRA, COLS)], where, own, near, far)
    parts = exchange(parts, "z")
    out, tile = call(sum_z_kernel, [(X * Y, ROWS + EXTRA, COLS), tile_shape], parts)

    def gather(out, tile):
        return exchange(out, ("y", "x")), z_gather(tile)

    row, col = gather(out, tile)
    out, tile, scale = call(square_kernel, [bcast_xy, tile_shape, (EXTRA, COLS)], where, row, *col, scratch=(Z, ROWS, COLS))
    srow, scol = gather(out, tile)
    out, tile, prow, ptile = call(
        poly_kernel,
        [bcast_xy, tile_shape, bcast_xy, tile_shape],
        where, row, srow, scale, *col, *scol, scratch=(Z, ROWS, COLS),
    )
    wrow, hcol = gather(out, tile)
    out, gtile, utile = call(
        shared_column_kernel, [bcast_xy, tile_shape, tile_shape], where, prow, wrow, *hcol, scratch=(Z, ROWS, COLS)
    )
    urow, gcol = gather(out, gtile)
    out, both = call(
        second_poly_kernel, [bcast_xy, tile_shape], where, urow, gtile, ptile, utile, *hcol, *gcol, scratch=(Z, ROWS, 2 * COLS)
    )
    prow, bothcol = gather(out, both)
    out, tile = call(
        shared_row_kernel, [bcast_xy, tile_shape], where, prow, *gcol, *bothcol, scratch=(Z, ROWS, 2 * COLS)
    )
    xrow, hcol = gather(out, tile)
    out, gtile, vtile = call(
        shared_column_kernel, [bcast_xy, tile_shape, tile_shape], where, prow, xrow, *hcol, scratch=(Z, ROWS, COLS)
    )
    vrow, gcol = gather(out, gtile)
    (q,) = call(last_kernel, [tile_shape], where, vrow, both, vtile, scale, *gcol, scratch=(Z, ROWS, COLS))

    across = exchange(jnp.broadcast_to(q[None, 128:], (X, 128, COLS)), "x")
    upper = jnp.stack(z_gather(q[:128]))
    upper = exchange(jnp.broadcast_to(upper[None], (X, *upper.shape)), "x")
    lower = z_gather(across)
    (step,) = call(
        apply_kernel, [(256, 512)], where, *rows, upper, *lower, scratch=(Z, 128, 512), flops=1_600_000_000
    )
    return moment[None], step[None]


def solution(mesh):
    torus = Mesh(
        mesh.devices.reshape(Z, X, Y, mesh.shape["rep"]),
        ("z", "x", "y", "rep"),
    )
    in_specs = (P("rep", None, ("z", "x"), "y"), P("rep", ("z", "x"), "y"))
    out_specs = (P("rep", ("z", "x"), "y"), P("rep", ("z", "x"), "y"))
    return jax.shard_map(
        per_device, mesh=torus, in_specs=in_specs, out_specs=out_specs, check_vma=False
    )
```

```python
import functools
import math

import jax
import jax.numpy as jnp
from jax import lax
from jax.experimental import pallas as pl
from jax.experimental.pallas import tpu as pltpu
from jax.sharding import Mesh
from jax.sharding import PartitionSpec as P

D = 2048
FF = 8192
Z, X, Y = 8, 4, 4
ROWS = D // Z
COLS = D // (X * Y)
EXTRA = 8

momentum_decay = 0.95
norm_spread = 2.56
linear = 3.4445
cubic = -4.775
quintic = 2.0315


f32, bf16 = jnp.float32, jnp.bfloat16
HBM = pl.BlockSpec(memory_space=pltpu.HBM)
VMEM = pl.BlockSpec(memory_space=pltpu.VMEM)
SMEM = pl.BlockSpec(memory_space=pltpu.SMEM)


def split(a):
    high = a.astype(bf16)
    rest = a - high.astype(f32)
    middle = rest.astype(bf16)
    return high, middle, (rest - middle.astype(f32)).astype(bf16)


def dot(a, b, dims=((1,), (0,))):
    return lax.dot_general(a, b, (dims, ((), ())), preferred_element_type=f32)


def product(a, b, dims=((1,), (0,))):
    a1, a2, a3 = split(a)
    b1, b2, b3 = split(b)
    n = b.shape[1]
    if n == COLS:
        pair = jnp.concatenate([b1, b2], 1)
        upper, lower = dot(a1, pair, dims), dot(a2, pair, dims)
        small = dot(a1, b3, dims) + (dot(a3, b1, dims) + lower[:, n:])
        return upper[:, :n] + (small + (upper[:, n:] + lower[:, :n]))
    small = dot(a1, b3, dims) + (dot(a3, b1, dims) + dot(a2, b2, dims))
    return dot(a1, b1, dims) + (small + (dot(a1, b2, dims) + dot(a2, b1, dims)))


def eye(first_row, first_col):
    rows = lax.broadcasted_iota(jnp.int32, (ROWS, COLS), 0) + first_row
    cols = lax.broadcasted_iota(jnp.int32, (ROWS, COLS), 1) + first_col
    return jnp.where(rows == cols, jnp.float32(linear), jnp.float32(0))


class Near:
    def __init__(self, array):
        self.array = array


class Out:
    def __init__(self, shape=None, count=None, operand=None, dtype=f32, again=None):
        self.shape, self.count, self.operand, self.dtype, self.again = shape, count, operand, dtype, again


def call(body, where, operands, outs, flops=800_000_000, scratch=(), limit=20):
    arrays, specs, scratches, plan = [where], [SMEM], [], []
    for operand in operands:
        if isinstance(operand, Near):
            plan.append(("near", len(arrays), 1))
            arrays.append(operand.array)
            specs.append(VMEM)
            continue
        group = operand if isinstance(operand, list) else [operand]
        shape = group[0].shape
        scratches.append(pltpu.VMEM((len(group), *shape) if isinstance(operand, list) else shape, group[0].dtype))
        plan.append(("list" if isinstance(operand, list) else "one", len(arrays), len(group)))
        arrays += [pltpu.with_memory_space_constraint(array, pltpu.HBM) for array in group]
        specs += [HBM] * len(group)
    loads = sum(count for kind, _, count in plan if kind != "near")
    shapes = []
    for out in outs:
        shape = out.shape
        if out.again is not None:
            shape = outs[out.again].shape
        elif out.operand is None:
            scratches.append(pltpu.VMEM(shape, out.dtype))
        elif operands[out.operand].__class__ is list:
            shape = (len(operands[out.operand]), *operands[out.operand][0].shape)
        else:
            shape = getattr(operands[out.operand], "array", operands[out.operand]).shape
        shapes.append(pltpu.HBM((out.count, *shape) if out.count else shape, out.dtype))
    stores = sum(out.count or 1 for out in outs)
    held = len(scratches)
    scratches += [pltpu.VMEM(shape, f32) for shape in scratch]
    scratches += [pltpu.SemaphoreType.DMA((max(loads, 1),)), pltpu.SemaphoreType.DMA((stores,))]

    def kernel(*refs):
        given, made, rest = refs[: len(arrays)], refs[len(arrays) : len(arrays) + len(outs)], refs[len(arrays) + len(outs) :]
        buffers, extra, (load_sem, store_sem) = list(rest[:held]), rest[held:-2], rest[-2:]
        views, copies = [], []
        for kind, first, count in plan:
            if kind == "near":
                views.append(given[first])
                continue
            buffer = buffers.pop(0)
            views.append(buffer)
            for n in range(count):
                target = buffer.at[n] if kind == "list" else buffer
                copies.append(pltpu.make_async_copy(given[first + n], target, load_sem.at[len(copies)]))
        for copy in copies:
            copy.start()
        for copy in copies:
            copy.wait()
        sources = []
        for out in outs:
            if out.again is not None:
                sources.append(sources[out.again])
            else:
                sources.append(buffers.pop(0) if out.operand is None else views[out.operand])
        groups, number = [], 0
        for out, source, ref in zip(outs, sources, made):
            targets = [ref.at[n] for n in range(out.count)] if out.count else [ref]
            groups.append([pltpu.make_async_copy(source, t, store_sem.at[number + n]) for n, t in enumerate(targets)])
            number += len(targets)
        for out, group in zip(outs, groups):
            if out.operand is not None:
                for copy in group:
                    copy.start()
        if body is not None:
            body(given[0], views, [v for v, out in zip(sources, outs) if out.operand is None and out.again is None], *extra)
        for out, group in zip(outs, groups):
            if out.operand is None:
                for copy in group:
                    copy.start()
        for group in groups:
            for copy in group:
                copy.wait()

    return pl.pallas_call(
        kernel,
        out_shape=shapes,
        in_specs=specs,
        out_specs=[HBM] * len(outs),
        scratch_shapes=scratches,
        compiler_params=pltpu.CompilerParams(vmem_limit_bytes=limit << 20),
        cost_estimate=pl.CostEstimate(flops=flops, bytes_accessed=4_000_000, transcendentals=0),
    )(*arrays)


def block(where, n):
    step = (n + 1) // 2
    return lax.rem(where[0] + Z + jnp.where(n % 2 == 1, -step, step), Z)


def tile_products(where, rows, cols):
    def step(n, totals):
        i = block(where, n)
        b = jnp.concatenate([col[n] for col in cols], 1)
        return tuple(
            t + product(jnp.concatenate([row(2 * i), row(2 * i + 1)], 1), b) for t, row in zip(totals, rows)
        )

    zero = jnp.zeros((ROWS, len(cols) * COLS), f32)
    totals = lax.fori_loop(0, Z, step, (zero,) * len(rows))
    return [t[:, c * COLS : (c + 1) * COLS] for t in totals for c in range(len(cols))]


def blocks_of(ref):
    return lambda j: ref[j, :ROWS, :]


def loop(count, body):
    def step(n, carry):
        body(n)
        return carry

    lax.fori_loop(0, count, step, 0)


def gram_own_kernel(where, operands, outs):
    (own,), (out,) = operands, outs
    mine = own[...]

    def part(n):
        columns = pl.ds(pl.multiple_of(n * 256, 256), 256)
        part = product(own[:, columns], mine, ((0,), (0,)))
        for x in range(X):
            out[x, columns, :] = part[:, x * COLS : (x + 1) * COLS]

    loop(2, part)
    squares = jnp.sum(mine * mine)
    for x in range(X):
        out[x, 512:, :] = jnp.full((EXTRA, COLS), squares, f32)


def gram_rest_kernel(where, operands, outs, others):
    own, before, after, upper, lower = operands
    out, high, low = outs
    others[0], others[1] = before[...], after[...]
    others[2, :128], others[2, 128:] = upper[...], lower[...]
    mine = own[...]

    def part(n):
        columns = pl.ds(pl.multiple_of(lax.rem(n, 2) * 256, 256), 256)
        part = product(others[n // 2, :, columns], mine, ((0,), (0,)))
        for x in range(X):
            out[x, pl.ds(pl.multiple_of(n * 256, 256), 256), :] = part[:, x * COLS : (x + 1) * COLS]

    loop(6, part)
    y = where[1] // X

    def keep(part, step):
        first, second, _ = split(part)
        for half in range(2):
            i = 2 * lax.rem(y + step, Y) + half
            high[i] = first[:, half * 256 : (half + 1) * 256]
            low[i] = second[:, half * 256 : (half + 1) * 256]

    keep(mine, 0)
    loop(3, lambda n: keep(others[n], jnp.where(n == 0, Y - 1, n)))


def sum_x_kernel(where, operands, outs, sums):
    own, rest = operands

    def total(parts, first, count):
        rows = slice(first, first + count)
        return (parts[0, rows] + parts[1, rows]) + (parts[2, rows] + parts[3, rows])

    y = where[1] // X
    for parts, first, step in ((own, 0, 0), (rest, 0, Y - 1), (rest, 512, 1), (rest, 1024, 2)):
        for half in range(2):
            z = 2 * lax.rem(y + step, Y) + half
            sums[z, :ROWS, :] = total(parts, first + half * ROWS, ROWS)
    extra = total(own, 512, EXTRA)
    for z in range(Z):
        sums[z, ROWS:, :] = extra
    for n, out in enumerate(outs):
        out[...] = sums[block(where, n)]


def sum_z_kernel(where, operands, outs):
    parts, (out, tile) = operands[0], outs
    total = parts[0]
    for n in range(1, len(parts)):
        total = total + parts[n]
    out[...] = total
    tile[...] = total[:ROWS]


def square_kernel(where, operands, outs):
    (row, col), (out, scale) = operands, outs
    squares = jnp.zeros((EXTRA, COLS), f32)
    for n in range(X * Y):
        squares = squares + row[n, ROWS:, :]
    squares = squares * (1.0 / X)
    scaling = jnp.sqrt(norm_spread * squares / D + 1.0)
    scale[...] = 1.0 / scaling
    inverse = jnp.max(1.0 / (scaling * scaling))
    (total,) = tile_products(where, [blocks_of(row)], [col])
    out[...] = total * (inverse * inverse)


def poly_kernel(where, operands, outs, pcol):
    srow, row, scale, col, scol = operands
    out, tile, prow, ptile = outs
    s = jnp.max(scale[...])
    inverse = s * s

    def poly_row(j):
        scaled = row[j, :ROWS, :] * inverse
        prow[j] = eye(where[0] * ROWS, j * COLS) + (cubic * scaled + quintic * srow[j])

    def poly_col(n):
        first = eye(block(where, n) * ROWS, where[1] * COLS)
        pcol[n] = first + (cubic * (col[n] * inverse) + quintic * scol[n])

    loop(X * Y, poly_row)
    loop(Z, poly_col)
    ptile[...] = pcol[0]
    h, w = tile_products(where, [blocks_of(row), blocks_of(prow)], [pcol])
    out[...] = w
    tile[...] = h * inverse


def shared_column_kernel(where, operands, outs):
    (right, left, col), (out, tile) = operands, outs
    tile[...], out[...] = tile_products(where, [blocks_of(left), blocks_of(right)], [col])


def second_poly_kernel(where, operands, outs):
    row, gtile, ptile, utile, hcol, col = operands
    out, tile = outs
    squared, times = tile_products(where, [blocks_of(row)], [hcol, col])
    first = eye(where[0] * ROWS, where[1] * COLS)
    out[...] = first + (cubic * gtile[...] + quintic * squared)
    tile[...] = linear * ptile[...] + (cubic * utile[...] + quintic * times)


def shared_row_kernel(where, operands, outs):
    row, col, other = operands
    out, tile = outs
    tile[...], out[...] = tile_products(where, [blocks_of(row)], [col, other])


def last_kernel(where, operands, outs):
    row, both, vtile, scale, col = operands
    upper, lower = outs
    (total,) = tile_products(where, [blocks_of(row)], [col])
    total = linear * both[...] + (cubic * vtile[...] + quintic * total)
    total = total * (jnp.max(scale[...]) * math.sqrt(FF))
    upper[...], lower[...] = total[:128], total[128:]


def apply_kernel(where, operands, outs):
    upper, high, low, lower = operands

    def step(n, total):
        i = block(where, n)
        first = jnp.concatenate([upper[x, n] for x in range(X)], 1)
        second = jnp.concatenate([lower[n, x] for x in range(X)], 1)
        b1, b2, _ = split(jnp.concatenate([first, second], 0))
        return total + (dot(high[i], b1) + (dot(high[i], b2) + dot(low[i], b1)))

    outs[0][...] = lax.fori_loop(0, Z, step, jnp.zeros((256, 512), f32))


def exchange(parts, axes):
    return lax.all_to_all(parts, axes, 0, 0, tiled=True)


def along_z(a, offset):
    return lax.ppermute(a, "z", [(i, (i - offset) % Z) for i in range(Z)])


def z_gather(tile):
    near = {o: along_z(tile, o) for o in (1, -1, 2, -2)}
    far = along_z(near[2], 2)
    return [tile, near[-1], near[1], near[-2], near[2], along_z(near[-2], -1), along_z(near[2], 1), far]


def z_scatter(parts):
    own, down1, up1, down2, up2, down3, up3, far = parts
    up2 = up2 + along_z(up3, -1) + along_z(far, -2)
    down2 = down2 + along_z(down3, 1)
    return [own, along_z(up1, -1), along_z(down1, 1), along_z(up2, -2), along_z(down2, 2)]


def per_device(grads, momentum):
    me = lax.axis_index("rep")
    theirs = lax.dynamic_index_in_dim(grads[0], 1 - me, 0, keepdims=False)
    mine = lax.dynamic_index_in_dim(grads[0], me, 0, keepdims=False)
    moment = momentum_decay * momentum[0] + (mine + lax.ppermute(theirs, "rep", [(0, 1), (1, 0)]))
    where = jnp.stack([lax.axis_index("z"), lax.axis_index("y") * X + lax.axis_index("x")]).astype(jnp.int32)

    up, down = [(i, (i + 1) % Y) for i in range(Y)], [(i, (i - 1) % Y) for i in range(Y)]
    before, after = lax.ppermute(moment, "y", up), lax.ppermute(moment, "y", down)
    upper, lower = lax.ppermute(before[:128], "y", up), lax.ppermute(after[128:], "y", down)
    (own,) = call(gram_own_kernel, where, [moment], [Out((X, 512 + EXTRA, COLS))])
    own = exchange(own, "x")
    rest, *rows = call(
        gram_rest_kernel,
        where,
        [moment, before, after, upper, lower],
        [Out((X, 1536, COLS)), Out((Z, ROWS, 256), dtype=bf16), Out((Z, ROWS, 256), dtype=bf16)],
        scratch=[(3, 256, 512)],
        flops=2_400_000_000,
    )
    rest = exchange(rest, "x")
    long_tile = (ROWS + EXTRA, COLS)
    parts = call(sum_x_kernel, where, [own, Near(rest)], [Out(long_tile)] * Z, scratch=[(Z, *long_tile)])
    tile, plane = (ROWS, COLS), X * Y
    out, gtile = call(sum_z_kernel, where, [z_scatter(parts)], [Out(long_tile, plane), Out(tile)])

    def gather(out, tile):
        return Near(exchange(out, ("y", "x"))), z_gather(tile)

    row, col = gather(out, gtile)
    out, stile, scale, row, col = call(
        square_kernel,
        where,
        [row, col],
        [Out(tile, plane), Out(again=0), Out((EXTRA, COLS)), Out(operand=0), Out(operand=1)],
    )
    srow, scol = gather(out, stile)
    out, htile, prow, ptile = call(
        poly_kernel,
        where,
        [srow, row, scale, col, scol],
        [Out(tile, plane), Out(tile), Out((plane, *tile)), Out(tile)],
        scratch=[(Z, *tile)],
    )
    wrow, hcol = gather(out, htile)
    out, utile, gtile, hcol = call(
        shared_column_kernel, where, [wrow, prow, hcol], [Out(tile, plane), Out(again=0), Out(tile), Out(operand=2)]
    )
    urow, gcol = gather(out, gtile)
    out, both, gcol = call(
        second_poly_kernel,
        where,
        [urow, gtile, ptile, utile, hcol, gcol],
        [Out(tile, plane), Out(tile), Out(operand=5)],
    )
    prow, bothcol = gather(out, both)
    out, htile, prow = call(
        shared_row_kernel, where, [prow, gcol, bothcol], [Out(tile, plane), Out(tile), Out(operand=0)]
    )
    xrow, hcol = gather(out, htile)
    out, vtile, gtile = call(
        shared_column_kernel, where, [xrow, prow, hcol], [Out(tile, plane), Out(again=0), Out(tile)]
    )
    vrow, gcol = gather(out, gtile)
    half = (128, COLS)
    upper, lower = call(
        last_kernel, where, [vrow, both, vtile, scale, gcol], [Out(half), Out(half, X)]
    )

    lower = exchange(lower, "x")
    (upper,) = call(None, where, [z_gather(upper)], [Out(operand=0, count=X)])
    upper = exchange(upper, "x")
    lower = z_gather(lower)
    (step,) = call(apply_kernel, where, [Near(upper), *rows, lower], [Out((256, 512))], flops=1_600_000_000)
    return moment[None], step[None]


def solution(mesh):
    torus = Mesh(
        mesh.devices.reshape(Z, X, Y, mesh.shape["rep"]),
        ("z", "x", "y", "rep"),
    )
    in_specs = (P("rep", None, ("z", "x"), "y"), P("rep", ("z", "x"), "y"))
    out_specs = (P("rep", ("z", "x"), "y"), P("rep", ("z", "x"), "y"))
    return jax.shard_map(
        per_device, mesh=torus, in_specs=in_specs, out_specs=out_specs, check_vma=False
    )
```

```python
import math

import jax
import jax.numpy as jnp
from jax import lax
from jax.experimental import pallas as pl
from jax.experimental.pallas import tpu as pltpu
from jax.sharding import Mesh
from jax.sharding import PartitionSpec as P


D = 2048
FF = 8192
Z, X, Y = 8, 4, 4
ROWS = D // Z
COLS = D // (X * Y)
EXTRA = 8

momentum_decay = 0.95
norm_spread = 2.56
linear = 3.4445
cubic = -4.775
quintic = 2.0315


f32, bf16 = jnp.float32, jnp.bfloat16

HBM = pl.BlockSpec(memory_space=pltpu.HBM)
VMEM = pl.BlockSpec(memory_space=pltpu.VMEM)
SMEM = pl.BlockSpec(memory_space=pltpu.SMEM)


def split(a):
    high = a.astype(bf16)
    rest = a - high.astype(f32)
    middle = rest.astype(bf16)
    return high, middle, (rest - middle.astype(f32)).astype(bf16)


def dot(a, b, dims=((1,), (0,))):
    return lax.dot_general(a, b, (dims, ((), ())), preferred_element_type=f32)


def product(a, b, dims=((1,), (0,))):
    a1, a2, a3 = split(a)
    b1, b2, b3 = split(b)
    n = b.shape[1]
    if n == COLS:
        pair = jnp.concatenate([b1, b2], 1)
        upper, lower = dot(a1, pair, dims), dot(a2, pair, dims)
        small = dot(a1, b3, dims) + (dot(a3, b1, dims) + lower[:, n:])
        return upper[:, :n] + (small + (upper[:, n:] + lower[:, :n]))
    small = dot(a1, b3, dims) + (dot(a3, b1, dims) + dot(a2, b2, dims))
    return dot(a1, b1, dims) + (small + (dot(a1, b2, dims) + dot(a2, b1, dims)))


def eye(first_row, first_col):
    rows = lax.broadcasted_iota(jnp.int32, (ROWS, COLS), 0) + first_row
    cols = lax.broadcasted_iota(jnp.int32, (ROWS, COLS), 1) + first_col
    return jnp.where(rows == cols, jnp.float32(linear), jnp.float32(0))


class Near:
    def __init__(self, array):
        self.array = array


class Out:
    def __init__(self, shape=None, count=None, operand=None, dtype=f32, again=None):
        self.shape, self.count, self.operand, self.dtype, self.again = shape, count, operand, dtype, again


def call(body, where, operands, outs, flops=800_000_000, scratch=(), limit=20, lazy=False):
    arrays, specs, scratches, plan = [where], [SMEM], [], []
    for operand in operands:
        if isinstance(operand, Near):
            plan.append(("near", len(arrays), 1))
            arrays.append(operand.array)
            specs.append(VMEM)
            continue
        group = operand if isinstance(operand, list) else [operand]
        shape = group[0].shape
        scratches.append(pltpu.VMEM((len(group), *shape) if isinstance(operand, list) else shape, group[0].dtype))
        plan.append(("list" if isinstance(operand, list) else "one", len(arrays), len(group)))
        arrays += [pltpu.with_memory_space_constraint(array, pltpu.HBM) for array in group]
        specs += [HBM] * len(group)
    loads = sum(count for kind, _, count in plan if kind != "near")
    shapes = []
    for out in outs:
        shape = out.shape
        if out.again is not None:
            shape = outs[out.again].shape
        elif out.operand is None:
            scratches.append(pltpu.VMEM(shape, out.dtype))
        elif operands[out.operand].__class__ is list:
            shape = (len(operands[out.operand]), *operands[out.operand][0].shape)
        else:
            shape = getattr(operands[out.operand], "array", operands[out.operand]).shape
        shapes.append(pltpu.HBM((out.count, *shape) if out.count else shape, out.dtype))
    stores = sum(out.count or 1 for out in outs)
    held = len(scratches)
    scratches += [pltpu.VMEM(shape, f32) for shape in scratch]
    scratches += [pltpu.SemaphoreType.DMA((max(loads, 1),)), pltpu.SemaphoreType.DMA((stores,))]

    def kernel(*refs):
        given, made, rest = refs[: len(arrays)], refs[len(arrays) : len(arrays) + len(outs)], refs[len(arrays) + len(outs) :]
        buffers, extra, (load_sem, store_sem) = list(rest[:held]), rest[held:-2], rest[-2:]
        views, copies, late = [], [], []
        for kind, first, count in plan:
            if kind == "near":
                views.append(given[first])
                continue
            buffer = buffers.pop(0)
            views.append(buffer)
            if lazy and kind == "list":
                late.append((given[first], buffer, len(copies), count))
            for n in range(count):
                target = buffer.at[n] if kind == "list" else buffer
                copies.append(pltpu.make_async_copy(given[first + n], target, load_sem.at[len(copies)]))
        for copy in copies:
            copy.start()
        held_back = {first + n for _, _, first, count in late for n in range(count)}
        for n, copy in enumerate(copies):
            if n not in held_back:
                copy.wait()

        def ready(n):
            for source, buffer, first, _ in late:
                pltpu.make_async_copy(source, buffer.at[n], load_sem.at[first + n]).wait()

        if lazy:
            extra = (*extra, ready)
        sources = []
        for out in outs:
            if out.again is not None:
                sources.append(sources[out.again])
            else:
                sources.append(buffers.pop(0) if out.operand is None else views[out.operand])
        groups, number = [], 0
        for out, source, ref in zip(outs, sources, made):
            targets = [ref.at[n] for n in range(out.count)] if out.count else [ref]
            groups.append([pltpu.make_async_copy(source, t, store_sem.at[number + n]) for n, t in enumerate(targets)])
            number += len(targets)
        for out, group in zip(outs, groups):
            if out.operand is not None and not (lazy and isinstance(operands[out.operand], list)):
                for copy in group:
                    copy.start()
        if body is not None:
            body(given[0], views, [v for v, out in zip(sources, outs) if out.operand is None and out.again is None], *extra)
        for out, group in zip(outs, groups):
            if out.operand is None or (lazy and isinstance(operands[out.operand], list)):
                for copy in group:
                    copy.start()
        for group in groups:
            for copy in group:
                copy.wait()

    return pl.pallas_call(
        kernel,
        out_shape=shapes,
        in_specs=specs,
        out_specs=[HBM] * len(outs),
        scratch_shapes=scratches,
        compiler_params=pltpu.CompilerParams(vmem_limit_bytes=limit << 20),
        cost_estimate=pl.CostEstimate(flops=flops, bytes_accessed=4_000_000, transcendentals=0),
    )(*arrays)


def block(where, n):
    step = (n + 1) // 2
    return lax.rem(where[0] + Z + jnp.where(n % 2 == 1, -step, step), Z)


def tile_products(where, rows, cols, ready=None):
    def step(n, totals):
        if ready is not None:
            ready(n)
        i = block(where, n)
        b = jnp.concatenate([col[n] for col in cols], 1)
        return tuple(
            t + product(jnp.concatenate([row(2 * i), row(2 * i + 1)], 1), b) for t, row in zip(totals, rows)
        )

    zero = jnp.zeros((ROWS, len(cols) * COLS), f32)
    totals = lax.fori_loop(0, Z, step, (zero,) * len(rows))
    return [t[:, c * COLS : (c + 1) * COLS] for t in totals for c in range(len(cols))]


def blocks_of(ref):
    return lambda j: ref[j, :ROWS, :]


def loop(count, body):
    def step(n, carry):
        body(n)
        return carry

    lax.fori_loop(0, count, step, 0)


def gram_own_kernel(where, operands, outs):
    (own,), (out,) = operands, outs
    mine = own[...]

    def part(n):
        columns = pl.ds(pl.multiple_of(n * 256, 256), 256)
        part = product(jnp.transpose(own[:, columns]), mine)
        for x in range(X):
            out[x, columns, :] = part[:, x * COLS : (x + 1) * COLS]

    loop(2, part)
    squares = jnp.sum(mine * mine)
    for x in range(X):
        out[x, 512:, :] = jnp.full((EXTRA, COLS), squares, f32)


def gather_rows(operands, others):
    _, before, after, upper, lower = operands
    others[0], others[1] = before[...], after[...]
    others[2, :128], others[2, 128:] = upper[...], lower[...]


def gram_rest_kernel(where, operands, outs, others):
    (out,) = outs
    gather_rows(operands, others)
    mine = operands[0][...]

    def part(n):
        columns = pl.ds(pl.multiple_of(lax.rem(n, 2) * 256, 256), 256)
        part = product(jnp.transpose(others[n // 2, :, columns]), mine)
        for x in range(X):
            out[x, pl.ds(pl.multiple_of(n * 256, 256), 256), :] = part[:, x * COLS : (x + 1) * COLS]

    loop(6, part)


def prepare_kernel(where, operands, outs, others):
    high, low = outs
    gather_rows(operands, others)
    y = where[1] // X

    def keep(part, step):
        first, second, _ = split(part)
        for half in range(2):
            i = 2 * lax.rem(y + step, Y) + half
            high[i] = first[:, half * 256 : (half + 1) * 256]
            low[i] = second[:, half * 256 : (half + 1) * 256]

    keep(operands[0][...], 0)
    loop(3, lambda n: keep(others[n], jnp.where(n == 0, Y - 1, n)))


def sum_x_kernel(where, operands, outs, sums):
    own, rest = operands

    def total(parts, first, count):
        rows = slice(first, first + count)
        return (parts[0, rows] + parts[1, rows]) + (parts[2, rows] + parts[3, rows])

    y = where[1] // X
    for parts, first, step in ((own, 0, 0), (rest, 0, Y - 1), (rest, 512, 1), (rest, 1024, 2)):
        for half in range(2):
            z = 2 * lax.rem(y + step, Y) + half
            sums[z, :ROWS, :] = total(parts, first + half * ROWS, ROWS)
    extra = total(own, 512, EXTRA)
    for z in range(Z):
        sums[z, ROWS:, :] = extra
    for n, out in enumerate(outs):
        out[...] = sums[block(where, n)]


def sum_z_kernel(where, operands, outs):
    parts, (out, tile) = operands[0], outs
    total = parts[0]
    for n in range(1, len(parts)):
        total = total + parts[n]
    out[...] = total
    tile[...] = total[:ROWS]


def square_kernel(where, operands, outs, ready):
    (row, col), (out, scale) = operands, outs
    squares = jnp.zeros((EXTRA, COLS), f32)
    for n in range(X * Y):
        squares = squares + row[n, ROWS:, :]
    squares = squares * (1.0 / X)
    scaling = jnp.sqrt(norm_spread * squares / D + 1.0)
    scale[...] = 1.0 / scaling
    inverse = jnp.max(1.0 / (scaling * scaling))
    (total,) = tile_products(where, [blocks_of(row)], [col], ready)
    out[...] = total * (inverse * inverse)


def poly_kernel(where, operands, outs, pcol):
    srow, row, scale, col, scol = operands
    out, tile, prow, ptile = outs
    s = jnp.max(scale[...])
    inverse = s * s

    def poly_row(j):
        scaled = row[j, :ROWS, :] * inverse
        prow[j] = eye(where[0] * ROWS, j * COLS) + (cubic * scaled + quintic * srow[j])

    def poly_col(n):
        first = eye(block(where, n) * ROWS, where[1] * COLS)
        pcol[n] = first + (cubic * (col[n] * inverse) + quintic * scol[n])

    loop(X * Y, poly_row)
    loop(Z, poly_col)
    ptile[...] = pcol[0]
    h, w = tile_products(where, [blocks_of(row), blocks_of(prow)], [pcol])
    out[...] = w
    tile[...] = h * inverse


def shared_column_kernel(where, operands, outs, ready):
    (right, left, col), (out, tile) = operands, outs
    tile[...], out[...] = tile_products(where, [blocks_of(left), blocks_of(right)], [col], ready)


def second_poly_kernel(where, operands, outs, ready):
    row, gtile, ptile, utile, hcol, col = operands
    out, tile = outs
    squared, times = tile_products(where, [blocks_of(row)], [hcol, col], ready)
    first = eye(where[0] * ROWS, where[1] * COLS)
    out[...] = first + (cubic * gtile[...] + quintic * squared)
    tile[...] = linear * ptile[...] + (cubic * utile[...] + quintic * times)


def shared_row_kernel(where, operands, outs, ready):
    row, col, other = operands
    out, tile = outs
    tile[...], out[...] = tile_products(where, [blocks_of(row)], [col, other], ready)


def last_kernel(where, operands, outs, ready):
    row, both, vtile, scale, col = operands
    upper, lower = outs
    (total,) = tile_products(where, [blocks_of(row)], [col], ready)
    total = linear * both[...] + (cubic * vtile[...] + quintic * total)
    total = total * (jnp.max(scale[...]) * math.sqrt(FF))
    upper[...], lower[...] = total[:128], total[128:]


def apply_kernel(where, operands, outs):
    upper, high, low, lower = operands

    def step(n, total):
        i = block(where, n)
        first = jnp.concatenate([upper[x, n] for x in range(X)], 1)
        second = jnp.concatenate([lower[n, x] for x in range(X)], 1)
        b1, b2, _ = split(jnp.concatenate([first, second], 0))
        return total + (dot(high[i], b1) + (dot(high[i], b2) + dot(low[i], b1)))

    outs[0][...] = lax.fori_loop(0, Z, step, jnp.zeros((256, 512), f32))


def exchange(parts, axes):
    return lax.all_to_all(parts, axes, 0, 0, tiled=True)


def along_z(a, offset):
    return lax.ppermute(a, "z", [(i, (i - offset) % Z) for i in range(Z)])


def z_gather(tile):
    near = {o: along_z(tile, o) for o in (1, -1, 2, -2)}
    far = along_z(near[2], 2)
    return [tile, near[-1], near[1], near[-2], near[2], along_z(near[-2], -1), along_z(near[2], 1), far]


def z_scatter(parts):
    own, down1, up1, down2, up2, down3, up3, far = parts
    up2 = up2 + along_z(up3, -1) + along_z(far, -2)
    down2 = down2 + along_z(down3, 1)
    return [own, along_z(up1, -1), along_z(down1, 1), along_z(up2, -2), along_z(down2, 2)]


def per_device(grads, momentum):
    me = lax.axis_index("rep")
    theirs = lax.dynamic_index_in_dim(grads[0], 1 - me, 0, keepdims=False)
    mine = lax.dynamic_index_in_dim(grads[0], me, 0, keepdims=False)
    moment = momentum_decay * momentum[0] + (mine + lax.ppermute(theirs, "rep", [(0, 1), (1, 0)]))
    where = jnp.stack([lax.axis_index("z"), lax.axis_index("y") * X + lax.axis_index("x")]).astype(jnp.int32)

    up, down = [(i, (i + 1) % Y) for i in range(Y)], [(i, (i - 1) % Y) for i in range(Y)]
    before, after = lax.ppermute(moment, "y", up), lax.ppermute(moment, "y", down)
    upper, lower = lax.ppermute(before[:128], "y", up), lax.ppermute(after[128:], "y", down)
    (own,) = call(gram_own_kernel, where, [moment], [Out((X, 512 + EXTRA, COLS))])
    own = exchange(own, "x")
    pieces = [moment, before, after, upper, lower]
    (rest,) = call(
        gram_rest_kernel, where, pieces, [Out((X, 1536, COLS))], scratch=[(3, 256, 512)], flops=2_400_000_000
    )
    rows = call(
        prepare_kernel, where, pieces, [Out((Z, ROWS, 256), dtype=bf16)] * 2, scratch=[(3, 256, 512)]
    )
    rest = exchange(rest, "x")
    long_tile = (ROWS + EXTRA, COLS)
    parts = call(sum_x_kernel, where, [own, Near(rest)], [Out(long_tile)] * Z, scratch=[(Z, *long_tile)])
    tile, plane = (ROWS, COLS), X * Y
    out, gtile = call(sum_z_kernel, where, [z_scatter(parts)], [Out(long_tile, plane), Out(tile)])

    def gather(out, tile):
        return Near(exchange(out, ("y", "x"))), z_gather(tile)

    row, col = gather(out, gtile)
    out, stile, scale, row, col = call(
        square_kernel,
        where,
        [row, col],
        [Out(tile, plane), Out(again=0), Out((EXTRA, COLS)), Out(operand=0), Out(operand=1)],
        lazy=True,
    )
    srow, scol = gather(out, stile)
    out, htile, prow, ptile = call(
        poly_kernel,
        where,
        [srow, row, scale, col, scol],
        [Out(tile, plane), Out(tile), Out((plane, *tile)), Out(tile)],
        scratch=[(Z, *tile)],
    )
    wrow, hcol = gather(out, htile)
    out, utile, gtile, hcol = call(
        shared_column_kernel, where, [wrow, prow, hcol], [Out(tile, plane), Out(again=0), Out(tile), Out(operand=2)], lazy=True
    )
    urow, gcol = gather(out, gtile)
    out, both, gcol = call(
        second_poly_kernel,
        where,
        [urow, gtile, ptile, utile, hcol, gcol],
        [Out(tile, plane), Out(tile), Out(operand=5)],
        lazy=True,
    )
    prow, bothcol = gather(out, both)
    out, htile, prow = call(
        shared_row_kernel, where, [prow, gcol, bothcol], [Out(tile, plane), Out(tile), Out(operand=0)], lazy=True
    )
    xrow, hcol = gather(out, htile)
    out, vtile, gtile = call(
        shared_column_kernel, where, [xrow, prow, hcol], [Out(tile, plane), Out(again=0), Out(tile)], lazy=True
    )
    vrow, gcol = gather(out, gtile)
    half = (128, COLS)
    upper, lower = call(
        last_kernel, where, [vrow, both, vtile, scale, gcol], [Out(half), Out(half, X)], lazy=True
    )

    lower = exchange(lower, "x")
    upper = z_gather(upper)
    lower = z_gather(lower)
    (upper,) = call(None, where, [upper], [Out(operand=0, count=X)])
    upper = exchange(upper, "x")
    (step,) = call(apply_kernel, where, [Near(upper), *rows, lower], [Out((256, 512))], flops=1_600_000_000)
    return moment[None], step[None]


def solution(mesh):
    torus = Mesh(
        mesh.devices.reshape(Z, X, Y, mesh.shape["rep"]),
        ("z", "x", "y", "rep"),
    )
    in_specs = (P("rep", None, ("z", "x"), "y"), P("rep", ("z", "x"), "y"))
    out_specs = (P("rep", ("z", "x"), "y"), P("rep", ("z", "x"), "y"))
    return jax.shard_map(
        per_device, mesh=torus, in_specs=in_specs, out_specs=out_specs, check_vma=False
    )
```

```python
import functools
import math

import jax
import jax.numpy as jnp
from jax import lax
from jax.experimental import pallas as pl
from jax.experimental.pallas import tpu as pltpu
from jax.sharding import Mesh
from jax.sharding import PartitionSpec as P

D = 2048
FF = 8192
Z, X, Y = 8, 4, 4
ROWS = D // Z
COLS = D // (X * Y)
EXTRA = 8

momentum_decay = 0.95
norm_spread = 2.56
linear = 3.4445
cubic = -4.775
quintic = 2.0315


f32, bf16 = jnp.float32, jnp.bfloat16
HBM = pl.BlockSpec(memory_space=pltpu.HBM)
VMEM = pl.BlockSpec(memory_space=pltpu.VMEM)
SMEM = pl.BlockSpec(memory_space=pltpu.SMEM)


def split(a):
    high = a.astype(bf16)
    rest = a - high.astype(f32)
    middle = rest.astype(bf16)
    return high, middle, (rest - middle.astype(f32)).astype(bf16)


def dot(a, b, dims=((1,), (0,))):
    return lax.dot_general(a, b, (dims, ((), ())), preferred_element_type=f32)


def product(a, b, dims=((1,), (0,))):
    a1, a2, a3 = split(a)
    b1, b2, b3 = split(b)
    n = b.shape[1]
    if n == COLS:
        pair = jnp.concatenate([b1, b2], 1)
        upper, lower = dot(a1, pair, dims), dot(a2, pair, dims)
        small = dot(a1, b3, dims) + (dot(a3, b1, dims) + lower[:, n:])
        return upper[:, :n] + (small + (upper[:, n:] + lower[:, :n]))
    small = dot(a1, b3, dims) + (dot(a3, b1, dims) + dot(a2, b2, dims))
    return dot(a1, b1, dims) + (small + (dot(a1, b2, dims) + dot(a2, b1, dims)))


def eye(first_row, first_col):
    rows = lax.broadcasted_iota(jnp.int32, (ROWS, COLS), 0) + first_row
    cols = lax.broadcasted_iota(jnp.int32, (ROWS, COLS), 1) + first_col
    return jnp.where(rows == cols, jnp.float32(linear), jnp.float32(0))


class Near:
    def __init__(self, array):
        self.array = array


class Out:
    def __init__(self, shape=None, count=None, operand=None, dtype=f32, again=None):
        self.shape, self.count, self.operand, self.dtype, self.again = shape, count, operand, dtype, again


def call(body, where, operands, outs, flops=800_000_000, scratch=(), limit=20):
    arrays, specs, scratches, plan = [where], [SMEM], [], []
    for operand in operands:
        if isinstance(operand, Near):
            plan.append(("near", len(arrays), 1))
            arrays.append(operand.array)
            specs.append(VMEM)
            continue
        group = operand if isinstance(operand, list) else [operand]
        shape = group[0].shape
        scratches.append(pltpu.VMEM((len(group), *shape) if isinstance(operand, list) else shape, group[0].dtype))
        plan.append(("list" if isinstance(operand, list) else "one", len(arrays), len(group)))
        arrays += [pltpu.with_memory_space_constraint(array, pltpu.HBM) for array in group]
        specs += [HBM] * len(group)
    loads = sum(count for kind, _, count in plan if kind != "near")
    shapes = []
    for out in outs:
        shape = out.shape
        if out.again is not None:
            shape = outs[out.again].shape
        elif out.operand is None:
            scratches.append(pltpu.VMEM(shape, out.dtype))
        elif operands[out.operand].__class__ is list:
            shape = (len(operands[out.operand]), *operands[out.operand][0].shape)
        else:
            shape = getattr(operands[out.operand], "array", operands[out.operand]).shape
        shapes.append(pltpu.HBM((out.count, *shape) if out.count else shape, out.dtype))
    stores = sum(out.count or 1 for out in outs)
    held = len(scratches)
    scratches += [pltpu.VMEM(shape, f32) for shape in scratch]
    scratches += [pltpu.SemaphoreType.DMA((max(loads, 1),)), pltpu.SemaphoreType.DMA((stores,))]

    def kernel(*refs):
        given, made, rest = refs[: len(arrays)], refs[len(arrays) : len(arrays) + len(outs)], refs[len(arrays) + len(outs) :]
        buffers, extra, (load_sem, store_sem) = list(rest[:held]), rest[held:-2], rest[-2:]
        views, copies = [], []
        for kind, first, count in plan:
            if kind == "near":
                views.append(given[first])
                continue
            buffer = buffers.pop(0)
            views.append(buffer)
            for n in range(count):
                target = buffer.at[n] if kind == "list" else buffer
                copies.append(pltpu.make_async_copy(given[first + n], target, load_sem.at[len(copies)]))
        for copy in copies:
            copy.start()
        for copy in copies:
            copy.wait()
        sources = []
        for out in outs:
            if out.again is not None:
                sources.append(sources[out.again])
            else:
                sources.append(buffers.pop(0) if out.operand is None else views[out.operand])
        groups, number = [], 0
        for out, source, ref in zip(outs, sources, made):
            targets = [ref.at[n] for n in range(out.count)] if out.count else [ref]
            groups.append([pltpu.make_async_copy(source, t, store_sem.at[number + n]) for n, t in enumerate(targets)])
            number += len(targets)
        for out, group in zip(outs, groups):
            if out.operand is not None:
                for copy in group:
                    copy.start()
        if body is not None:
            body(given[0], views, [v for v, out in zip(sources, outs) if out.operand is None and out.again is None], *extra)
        for out, group in zip(outs, groups):
            if out.operand is None:
                for copy in group:
                    copy.start()
        for group in groups:
            for copy in group:
                copy.wait()

    return pl.pallas_call(
        kernel,
        out_shape=shapes,
        in_specs=specs,
        out_specs=[HBM] * len(outs),
        scratch_shapes=scratches,
        compiler_params=pltpu.CompilerParams(vmem_limit_bytes=limit << 20),
        cost_estimate=pl.CostEstimate(flops=flops, bytes_accessed=4_000_000, transcendentals=0),
    )(*arrays)


def block(where, n):
    step = (n + 1) // 2
    return lax.rem(where[0] + Z + jnp.where(n % 2 == 1, -step, step), Z)


def tile_products(where, rows, cols):
    def step(n, totals):
        i = block(where, n)
        b = jnp.concatenate([col[n] for col in cols], 1)
        return tuple(
            t + product(jnp.concatenate([row(2 * i), row(2 * i + 1)], 1), b) for t, row in zip(totals, rows)
        )

    zero = jnp.zeros((ROWS, len(cols) * COLS), f32)
    totals = lax.fori_loop(0, Z, step, (zero,) * len(rows))
    return [t[:, c * COLS : (c + 1) * COLS] for t in totals for c in range(len(cols))]


def blocks_of(ref):
    return lambda j: ref[j, :ROWS, :]


def loop(count, body):
    def step(n, carry):
        body(n)
        return carry

    lax.fori_loop(0, count, step, 0)


def gram_own_kernel(where, operands, outs):
    (own,), (out,) = operands, outs
    mine = own[...]

    def part(n):
        columns = pl.ds(pl.multiple_of(n * 256, 256), 256)
        part = product(jnp.transpose(own[:, columns]), mine)
        for x in range(X):
            out[x, columns, :] = part[:, x * COLS : (x + 1) * COLS]

    loop(2, part)
    squares = jnp.sum(mine * mine)
    for x in range(X):
        out[x, 512:, :] = jnp.full((EXTRA, COLS), squares, f32)


def gram_rest_kernel(where, operands, outs, others):
    own, before, after, upper, lower = operands
    out, high, low = outs
    others[0], others[1] = before[...], after[...]
    others[2, :128], others[2, 128:] = upper[...], lower[...]
    mine = own[...]

    def part(n):
        columns = pl.ds(pl.multiple_of(lax.rem(n, 2) * 256, 256), 256)
        part = product(jnp.transpose(others[n // 2, :, columns]), mine)
        for x in range(X):
            out[x, pl.ds(pl.multiple_of(n * 256, 256), 256), :] = part[:, x * COLS : (x + 1) * COLS]

    loop(6, part)
    y = where[1] // X

    def keep(part, step):
        first, second, _ = split(part)
        for half in range(2):
            i = 2 * lax.rem(y + step, Y) + half
            high[i] = first[:, half * 256 : (half + 1) * 256]
            low[i] = second[:, half * 256 : (half + 1) * 256]

    keep(mine, 0)
    loop(3, lambda n: keep(others[n], jnp.where(n == 0, Y - 1, n)))


def sum_x_kernel(where, operands, outs, sums):
    own, rest = operands

    def total(parts, first, count):
        rows = slice(first, first + count)
        return (parts[0, rows] + parts[1, rows]) + (parts[2, rows] + parts[3, rows])

    y = where[1] // X
    for parts, first, step in ((own, 0, 0), (rest, 0, Y - 1), (rest, 512, 1), (rest, 1024, 2)):
        for half in range(2):
            z = 2 * lax.rem(y + step, Y) + half
            sums[z, :ROWS, :] = total(parts, first + half * ROWS, ROWS)
    extra = total(own, 512, EXTRA)
    for z in range(Z):
        sums[z, ROWS:, :] = extra
    for n, out in enumerate(outs):
        out[...] = sums[block(where, n)]


def sum_z_kernel(where, operands, outs):
    parts, (out, tile) = operands[0], outs
    total = parts[0]
    for n in range(1, len(parts)):
        total = total + parts[n]
    out[...] = total
    tile[...] = total[:ROWS]


def square_kernel(where, operands, outs):
    (row, col), (out, scale) = operands, outs
    squares = jnp.zeros((EXTRA, COLS), f32)
    for n in range(X * Y):
        squares = squares + row[n, ROWS:, :]
    squares = squares * (1.0 / X)
    scaling = jnp.sqrt(norm_spread * squares / D + 1.0)
    scale[...] = 1.0 / scaling
    inverse = jnp.max(1.0 / (scaling * scaling))
    (total,) = tile_products(where, [blocks_of(row)], [col])
    out[...] = total * (inverse * inverse)


def poly_kernel(where, operands, outs, pcol):
    srow, row, scale, col, scol = operands
    out, tile, prow, ptile = outs
    s = jnp.max(scale[...])
    inverse = s * s

    def poly_row(j):
        scaled = row[j, :ROWS, :] * inverse
        prow[j] = eye(where[0] * ROWS, j * COLS) + (cubic * scaled + quintic * srow[j])

    def poly_col(n):
        first = eye(block(where, n) * ROWS, where[1] * COLS)
        pcol[n] = first + (cubic * (col[n] * inverse) + quintic * scol[n])

    loop(X * Y, poly_row)
    loop(Z, poly_col)
    ptile[...] = pcol[0]
    h, w = tile_products(where, [blocks_of(row), blocks_of(prow)], [pcol])
    out[...] = w
    tile[...] = h * inverse


def shared_column_kernel(where, operands, outs):
    (right, left, col), (out, tile) = operands, outs
    tile[...], out[...] = tile_products(where, [blocks_of(left), blocks_of(right)], [col])


def second_poly_kernel(where, operands, outs):
    row, gtile, ptile, utile, hcol, col = operands
    out, tile = outs
    squared, times = tile_products(where, [blocks_of(row)], [hcol, col])
    first = eye(where[0] * ROWS, where[1] * COLS)
    out[...] = first + (cubic * gtile[...] + quintic * squared)
    tile[...] = linear * ptile[...] + (cubic * utile[...] + quintic * times)


def shared_row_kernel(where, operands, outs):
    row, col, other = operands
    out, tile = outs
    tile[...], out[...] = tile_products(where, [blocks_of(row)], [col, other])


def last_kernel(where, operands, outs):
    row, both, vtile, scale, col = operands
    upper, lower = outs
    (total,) = tile_products(where, [blocks_of(row)], [col])
    total = linear * both[...] + (cubic * vtile[...] + quintic * total)
    total = total * (jnp.max(scale[...]) * math.sqrt(FF))
    upper[...], lower[...] = total[:128], total[128:]


def apply_kernel(where, operands, outs):
    upper, high, low, lower = operands

    def step(n, total):
        i = block(where, n)
        first = jnp.concatenate([upper[x, n] for x in range(X)], 1)
        second = jnp.concatenate([lower[n, x] for x in range(X)], 1)
        b1, b2, _ = split(jnp.concatenate([first, second], 0))
        return total + (dot(high[i], b1) + (dot(high[i], b2) + dot(low[i], b1)))

    outs[0][...] = lax.fori_loop(0, Z, step, jnp.zeros((256, 512), f32))


def exchange(parts, axes):
    return lax.all_to_all(parts, axes, 0, 0, tiled=True)


def along_z(a, offset):
    return lax.ppermute(a, "z", [(i, (i - offset) % Z) for i in range(Z)])


def z_gather(tile):
    near = {o: along_z(tile, o) for o in (1, -1, 2, -2)}
    far = along_z(near[2], 2)
    return [tile, near[-1], near[1], near[-2], near[2], along_z(near[-2], -1), along_z(near[2], 1), far]


def z_scatter(parts):
    own, down1, up1, down2, up2, down3, up3, far = parts
    up2 = up2 + along_z(up3, -1) + along_z(far, -2)
    down2 = down2 + along_z(down3, 1)
    return [own, along_z(up1, -1), along_z(down1, 1), along_z(up2, -2), along_z(down2, 2)]


def per_device(grads, momentum):
    me = lax.axis_index("rep")
    theirs = lax.dynamic_index_in_dim(grads[0], 1 - me, 0, keepdims=False)
    mine = lax.dynamic_index_in_dim(grads[0], me, 0, keepdims=False)
    moment = momentum_decay * momentum[0] + (mine + lax.ppermute(theirs, "rep", [(0, 1), (1, 0)]))
    where = jnp.stack([lax.axis_index("z"), lax.axis_index("y") * X + lax.axis_index("x")]).astype(jnp.int32)

    up, down = [(i, (i + 1) % Y) for i in range(Y)], [(i, (i - 1) % Y) for i in range(Y)]
    before, after = lax.ppermute(moment, "y", up), lax.ppermute(moment, "y", down)
    upper, lower = lax.ppermute(before[:128], "y", up), lax.ppermute(after[128:], "y", down)
    (own,) = call(gram_own_kernel, where, [moment], [Out((X, 512 + EXTRA, COLS))])
    own = exchange(own, "x")
    rest, *rows = call(
        gram_rest_kernel,
        where,
        [moment, before, after, upper, lower],
        [Out((X, 1536, COLS)), Out((Z, ROWS, 256), dtype=bf16), Out((Z, ROWS, 256), dtype=bf16)],
        scratch=[(3, 256, 512)],
        flops=2_400_000_000,
    )
    rest = exchange(rest, "x")
    long_tile = (ROWS + EXTRA, COLS)
    parts = call(sum_x_kernel, where, [own, Near(rest)], [Out(long_tile)] * Z, scratch=[(Z, *long_tile)])
    tile, plane = (ROWS, COLS), X * Y
    out, gtile = call(sum_z_kernel, where, [z_scatter(parts)], [Out(long_tile, plane), Out(tile)])

    def gather(out, tile):
        return Near(exchange(out, ("y", "x"))), z_gather(tile)

    row, col = gather(out, gtile)
    out, stile, scale, row, col = call(
        square_kernel,
        where,
        [row, col],
        [Out(tile, plane), Out(again=0), Out((EXTRA, COLS)), Out(operand=0), Out(operand=1)],
    )
    srow, scol = gather(out, stile)
    out, htile, prow, ptile = call(
        poly_kernel,
        where,
        [srow, row, scale, col, scol],
        [Out(tile, plane), Out(tile), Out((plane, *tile)), Out(tile)],
        scratch=[(Z, *tile)],
    )
    wrow, hcol = gather(out, htile)
    out, utile, gtile, hcol = call(
        shared_column_kernel, where, [wrow, prow, hcol], [Out(tile, plane), Out(again=0), Out(tile), Out(operand=2)]
    )
    urow, gcol = gather(out, gtile)
    out, both, gcol = call(
        second_poly_kernel,
        where,
        [urow, gtile, ptile, utile, hcol, gcol],
        [Out(tile, plane), Out(tile), Out(operand=5)],
    )
    prow, bothcol = gather(out, both)
    out, htile, prow = call(
        shared_row_kernel, where, [prow, gcol, bothcol], [Out(tile, plane), Out(tile), Out(operand=0)]
    )
    xrow, hcol = gather(out, htile)
    out, vtile, gtile = call(
        shared_column_kernel, where, [xrow, prow, hcol], [Out(tile, plane), Out(again=0), Out(tile)]
    )
    vrow, gcol = gather(out, gtile)
    half = (128, COLS)
    upper, lower = call(
        last_kernel, where, [vrow, both, vtile, scale, gcol], [Out(half), Out(half, X)]
    )

    lower = exchange(lower, "x")
    (upper,) = call(None, where, [z_gather(upper)], [Out(operand=0, count=X)])
    upper = exchange(upper, "x")
    lower = z_gather(lower)
    (step,) = call(apply_kernel, where, [Near(upper), *rows, lower], [Out((256, 512))], flops=1_600_000_000)
    return moment[None], step[None]


def solution(mesh):
    torus = Mesh(
        mesh.devices.reshape(Z, X, Y, mesh.shape["rep"]),
        ("z", "x", "y", "rep"),
    )
    in_specs = (P("rep", None, ("z", "x"), "y"), P("rep", ("z", "x"), "y"))
    out_specs = (P("rep", ("z", "x"), "y"), P("rep", ("z", "x"), "y"))
    return jax.shard_map(
        per_device, mesh=torus, in_specs=in_specs, out_specs=out_specs, check_vma=False
    )
```
